1024 devices in a mesh: ep: 32 (over z, core), tp: 32 (over y, x).
Axes of the slice: x: 4, y: 8, z: 16, core: 2. Of those that a mesh axis runs over, the one named last changes fastest.
Arguments:
- tokens: bfloat16 [1536, 2048], P('ep', 'tp'), may hold values from -64 to 64
- mix_gain: float32 [2048], replicated, may hold values from 0.1 to 1.9
- w_gate_z: bfloat16 [2048, 2048], P(None, 'tp'), may hold values from -0.125 to 0.125
- w_value_x: bfloat16 [2048, 2048], P(None, 'tp'), may hold values from -0.125 to 0.125
- w_key_b: bfloat16 [2048, 256], replicated, may hold values from -0.125 to 0.125
- w_query_c: bfloat16 [2048, 256], replicated, may hold values from -0.125 to 0.125
- w_step: bfloat16 [2048, 32], replicated, may hold values from -0.125 to 0.125
- step_bias: float32 [32], replicated, may hold values from -2 to 1
- decay_log: float32 [32], replicated, may hold values from -3 to 1.4
- skip_gain: float32 [32], replicated, may hold values from 0.1 to 1.9
- conv_x_weight: bfloat16 [4, 2048], P(None, 'tp'), may hold values from -3 to 3
- conv_b_weight: bfloat16 [4, 256], replicated, may hold values from -3 to 3
- conv_c_weight: bfloat16 [4, 256], replicated, may hold values from -3 to 3
- window_x: bfloat16 [1536, 3, 2048], P('ep', None, 'tp'), may hold values from -6 to 6
- window_b: bfloat16 [1536, 3, 256], P('ep'), may hold values from -6 to 6
- window_c: bfloat16 [1536, 3, 256], P('ep'), may hold values from -6 to 6
- ssm_state: float32 [1536, 32, 64, 128], P('ep', 'tp'), may hold values from -2 to 2
- head_gain: float32 [2048], P('tp'), may hold values from 0.1 to 1.9
- w_out: bfloat16 [2048, 2048], P('tp'), may hold values from -0.25 to 0.25
- ffn_gain: float32 [2048], replicated, may hold values from 0.1 to 1.9
- route_ids: int32 [1536, 2], P('ep'), may hold values from 0 to 127, all different within a row; in each aligned block of 48 rows (0 to 47, 48 to 95, ...) at most 2 rows name the same one
- route_weights: float32 [1536, 2], P('ep'), may hold values from 0.05 to 1
- expert_gate: bfloat16 [32, 2048, 4096], P('ep', None, 'tp'), may hold values from -0.125 to 0.125
- expert_up: bfloat16 [32, 2048, 4096], P('ep', None, 'tp'), may hold values from -0.125 to 0.125
- expert_down: bfloat16 [32, 4096, 2048], P('ep', 'tp'), may hold values from -0.375 to 0.375
Outputs:
- layer_out: bfloat16 [1536, 2048], P('ep', 'tp')
The draws below stay inside these ranges and needn't reach their ends.
Inputs may be any that keep to these rules, and one draw needn't show every extreme that they name: `route_ids`: each row names 2 different experts. Within the rows of one index of ep (aligned blocks of 48 rows) no expert is named by more than 2 rows, a bound that some block reaches.
All inputs are finite; a program needn't handle non-finite values.
Results may differ from the reference program's by a relative error of at most 0.009.
Values may be sent and summed in bfloat16 or wider, within the bound.
A program may use at most 32 MiB of HBM per device.

```python
import math
import jax
import jax.numpy as jnp
import numpy as np
from jax import lax

D = 2048
HEADS = 32
HEAD_DIM = 64
STATE = 128
GROUPS = 2
CONV = 4
FE = 1024
EXP_IN = 4
TOPK = 2
SEQ_DEV = 48
SSD_W = 2048
GN = 256
SEQS = 1536
SETS = 32
EXPERTS = 128
SET_UNITS = 4096
CAP = 2
N_EP = 32


def draw_tokens(key, part):
    base_key = jax.random.fold_in(key, 11)
    row_key, column_key, body_key = jax.random.split(base_key, 3)
    row_scale = jnp.exp(jax.random.uniform(row_key, (SEQS, 1), jnp.float32, math.log(0.3), math.log(3.0)))
    column_scale = jnp.exp(jax.random.uniform(column_key, (1, D), jnp.float32, math.log(0.3), math.log(3.0)))
    pattern = jax.random.normal(body_key, (SEQS, D), jnp.float32)
    pattern = jnp.clip(pattern, -6.0, 6.0)
    return (pattern * row_scale * column_scale).astype(jnp.bfloat16)


def raised(entries, stream_key, source, target, shards_of, factor):
    owner, partner = [(jnp.arange(entries.shape[axis_at]) // (entries.shape[axis_at] // shards_of)).reshape([-1 if axis == axis_at else 1 for axis in range(entries.ndim)]) for axis_at in (source, target)]
    chosen = jax.random.permutation(stream_key, shards_of)[partner]
    strong = (owner == chosen) | (owner == (partner + shards_of // 2) % shards_of)
    return jnp.where(strong, factor * entries, entries)


def steps_of(rng, dims, shards, low, top_value):
    factor_of = 1.0
    for axis_at, parts in shards:
        heights = jax.random.uniform(jax.random.fold_in(jax.random.fold_in(rng, 6), axis_at), (parts,), jnp.float32, low / len(shards), top_value / len(shards))
        factor_of = factor_of * jnp.repeat(jnp.exp(heights), dims[axis_at] // parts).reshape((-1,) + (1,) * (len(dims) - 1 - axis_at))
    return factor_of


def deal_out(stream_key, own, number, rows, number_of, top, bound, slope):
    ranking = jax.random.permutation(stream_key, number_of)
    crowded, usual = load_shares(number_of, rows * top, bound, slope, True), load_shares(number_of, rows * top, bound, slope, False)
    places = jnp.arange(number_of)

    def named(lengths, offset_by):
        used = int((lengths > 0).sum())
        fixed = max(1, used // 4)
        moved = fixed + (places - fixed + offset_by * (used - fixed)) % max(1, number_of - fixed)
        return jnp.zeros((number_of,), jnp.int32).at[ranking[jnp.where(places < fixed, places, moved)]].set(jnp.asarray(lengths, jnp.int32))

    lengths = jnp.where(number % 4 == 0, named(crowded, number // 4), named(usual, number - number // 4 - 1))
    mixed = jax.random.permutation(jax.random.fold_in(own, 3), number_of)
    source_of, taker = mixed[0:number_of // 2 * 2:2], mixed[1:number_of // 2 * 2:2]
    margin = jnp.minimum(lengths[source_of] - 1, bound - lengths[taker]) // 2
    margin = jnp.where((source_of == ranking[0]) | (taker == ranking[0]) | (lengths[taker] == 0), 0, jnp.maximum(margin, 0))
    moved = jax.random.randint(jax.random.fold_in(own, 4), (number_of // 2,), 0, 1 << 20) % (margin + 1)
    lengths = lengths.at[source_of].add(-moved).at[taker].add(moved)
    labels = jnp.searchsorted(jnp.cumsum(lengths), jnp.arange(rows * top), side="right").astype(jnp.int32)
    table = labels.reshape(top, rows).T
    table = table[jax.random.permutation(jax.random.fold_in(own, 1), rows)]
    offset_by = jax.random.randint(jax.random.fold_in(own, 2), (rows, 1), 0, top)
    return jnp.take_along_axis(table, (jnp.arange(top)[None, :] + offset_by) % top, axis=1)


def load_shares(amount, total, reach, lean, full):
    portions = [(1 << 20) // math.isqrt(rank ** lean) + 1 for rank in range(1, amount + 1)]
    largest = reach if full else min(reach, max(-(-total // amount), total * portions[0] // sum(portions)))
    least = 1 if total - largest >= amount - 1 else 0
    given, rest = [largest] + [least] * (amount - 1), total - largest - least * (amount - 1)
    while rest > 0:
        free = [i for i in range(1, amount) if given[i] < largest] or [i for i in range(1, amount) if given[i] < reach]
        mass, left = sum([portions[i] for i in free]), rest
        for i in free:
            addition = min(reach - given[i], max(1, left * portions[i] // mass), rest)
            given[i] = given[i] + addition
            rest = rest - addition
    return np.array(given)


def noise(own_key, dims, width, limit, shards=(), kind=jnp.bfloat16):
    array = jax.random.normal(own_key, dims, jnp.float32) * width
    if len(shards) > 0:
        array = steps_of(own_key, dims, shards, -0.22, 0.18) * array
    return jnp.clip(array, min=-limit, max=limit).astype(kind)


def heavy_noise(stream_key, extent, spread, reach, pieces, heavy, held_as=jnp.bfloat16):
    entries = spread * jax.random.normal(stream_key, extent, jnp.float32)
    if pieces:
        entries = entries * steps_of(stream_key, extent, pieces, -0.22, 0.18)
    return jnp.clip(raised(entries, jax.random.fold_in(stream_key, 3), *heavy), -reach, reach).astype(held_as)


def setup_inputs(seed: int = 0) -> dict:
    arg_keys = jax.random.split(jax.random.key(seed), 26)
    tokens = draw_tokens(jax.random.fold_in(arg_keys[25], 71), 0)
    mix_gain = jnp.clip(1.0 + 0.18 * jax.random.normal(arg_keys[1], (D,), jnp.float32), 0.1, 1.9)
    w_gate_z = noise(arg_keys[2], (D, SSD_W), D ** -0.5, 0.125, ((1, 32),))
    w_value_x = noise(arg_keys[3], (D, SSD_W), D ** -0.5, 0.125, ((1, 32),))
    w_key_b = noise(arg_keys[4], (D, GN), D ** -0.5, 0.125)
    w_query_c = noise(arg_keys[5], (D, GN), D ** -0.5, 0.125)
    w_step = noise(arg_keys[6], (D, HEADS), D ** -0.5, 0.125)
    step_bias = jnp.clip(jax.random.uniform(arg_keys[7], (HEADS,), jnp.float32, -2.0, 1.0), -2.0, 1.0)
    decay_log = jnp.clip(jax.random.uniform(arg_keys[8], (HEADS,), jnp.float32, -3.0, 1.4), -3.0, 1.4)
    skip_gain = jnp.clip(1.0 + 0.18 * jax.random.normal(arg_keys[9], (HEADS,), jnp.float32), 0.1, 1.9)
    conv_x_weight = noise(arg_keys[10], (CONV, SSD_W), CONV ** -0.5, 3.0, ((1, 32),))
    conv_b_weight = noise(arg_keys[11], (CONV, GN), CONV ** -0.5, 3.0)
    conv_c_weight = noise(arg_keys[12], (CONV, GN), CONV ** -0.5, 3.0)
    window_x = noise(arg_keys[13], (SEQS, CONV - 1, SSD_W), 1.0, 6.0, ((0, 32), (2, 32)))
    window_b = noise(arg_keys[14], (SEQS, CONV - 1, GN), 1.0, 6.0, ((0, 32),))
    window_c = noise(arg_keys[15], (SEQS, CONV - 1, GN), 1.0, 6.0, ((0, 32),))
    ssm_state = noise(arg_keys[16], (SEQS, HEADS, HEAD_DIM, STATE), 0.3, 2.0, ((0, 32), (1, 32)), jnp.float32)
    head_gain = jnp.clip(1.0 + 0.18 * jax.random.normal(arg_keys[17], (SSD_W,), jnp.float32), 0.1, 1.9)
    w_out = heavy_noise(arg_keys[18], (SSD_W, D), SSD_W ** -0.5, 0.25, ((0, 32),), (0, 1, 32, 2.75))
    ffn_gain = jnp.clip(1.0 + 0.18 * jax.random.normal(arg_keys[19], (D,), jnp.float32), 0.1, 1.9)
    route_ids_keys = jax.random.split(jax.random.fold_in(arg_keys[20], 1), SEQS // SEQ_DEV)
    route_ids_turns = jax.random.permutation(jax.random.fold_in(arg_keys[20], 3), SEQS // SEQ_DEV)
    route_ids = jax.vmap(lambda own, number: deal_out(jax.random.fold_in(arg_keys[20], 2), own, number, SEQ_DEV, EXPERTS, TOPK, CAP, 2))(route_ids_keys, route_ids_turns).reshape((SEQS, TOPK))
    route_weights = jnp.clip(0.05 + 0.95 * jax.random.uniform(arg_keys[21], (SEQS, TOPK), jnp.float32) ** steps_of(arg_keys[21], (SEQS, TOPK), ((0, 32),), -0.2, 0.2), 0.05, 1.0)
    expert_gate = noise(arg_keys[22], (SETS, D, SET_UNITS), D ** -0.5, 0.125, ((0, 32), (2, 32)))
    expert_up = noise(arg_keys[23], (SETS, D, SET_UNITS), D ** -0.5, 0.125, ((0, 32), (2, 32)))
    expert_down = heavy_noise(arg_keys[24], (SETS, SET_UNITS, D), FE ** -0.5, 0.375, ((0, 32), (1, 32)), (1, 2, 32, 2.75))
    return {"tokens": tokens, "mix_gain": mix_gain, "w_gate_z": w_gate_z, "w_value_x": w_value_x, "w_key_b": w_key_b, "w_query_c": w_query_c, "w_step": w_step, "step_bias": step_bias, "decay_log": decay_log, "skip_gain": skip_gain, "conv_x_weight": conv_x_weight, "conv_b_weight": conv_b_weight, "conv_c_weight": conv_c_weight, "window_x": window_x, "window_b": window_b, "window_c": window_c, "ssm_state": ssm_state, "head_gain": head_gain, "w_out": w_out, "ffn_gain": ffn_gain, "route_ids": route_ids, "route_weights": route_weights, "expert_gate": expert_gate, "expert_up": expert_up, "expert_down": expert_down}


norm_epsilon = 1e-06

def row_norm(arr_values, norm_gain):
    widened = arr_values.astype(jnp.float32)
    return widened * lax.rsqrt(lax.optimization_barrier(jnp.mean(widened * widened, axis=-1, keepdims=True)) + norm_epsilon) * norm_gain

def short_conv(window, fresh_row, weight):
    conv_taps = weight.astype(jnp.float32)
    summed = lax.optimization_barrier(jnp.sum(window.astype(jnp.float32) * conv_taps[:-1][None], axis=1)) + fresh_row * conv_taps[-1]
    return jax.nn.silu(summed)

def product(left, right):
    return jnp.dot(left, right, preferred_element_type=jnp.float32)

def reference(tokens, mix_gain, w_gate_z, w_value_x, w_key_b, w_query_c, w_step, step_bias, decay_log, skip_gain, conv_x_weight, conv_b_weight, conv_c_weight, window_x, window_b, window_c, ssm_state, head_gain, w_out, ffn_gain, route_ids, route_weights, expert_gate, expert_up, expert_down):
    seq_count = tokens.shape[0]
    normed = row_norm(tokens, mix_gain).astype(jnp.bfloat16)
    gate_z = product(normed, w_gate_z)
    values = short_conv(window_x, product(normed, w_value_x), conv_x_weight)
    keys = short_conv(window_b, product(normed, w_key_b), conv_b_weight)
    queries = short_conv(window_c, product(normed, w_query_c), conv_c_weight)
    step_size = jax.nn.softplus(product(normed, w_step) + step_bias)
    decay_heads = jnp.exp(-step_size * jnp.exp(decay_log))
    per_group = HEADS // GROUPS
    value_heads = values.reshape(seq_count, HEADS, HEAD_DIM)
    key_heads = jnp.repeat(keys.reshape(seq_count, GROUPS, STATE), per_group, axis=1)
    query_heads = jnp.repeat(queries.reshape(seq_count, GROUPS, STATE), per_group, axis=1)
    new_state = decay_heads[:, :, None, None] * ssm_state + (step_size[:, :, None] * value_heads)[..., None] * key_heads[:, :, None, :]
    read_out = jnp.einsum('shpn,shn->shp', new_state, query_heads, precision=lax.Precision.HIGHEST)
    read_out = read_out + skip_gain[None, :, None] * value_heads
    gated = read_out * jax.nn.silu(gate_z.reshape(seq_count, HEADS, HEAD_DIM))
    gated = gated * lax.rsqrt(lax.optimization_barrier(jnp.mean(gated * gated, axis=-1, keepdims=True)) + norm_epsilon)
    mixed_heads = (gated * head_gain.reshape(HEADS, HEAD_DIM)).reshape(seq_count, SSD_W).astype(jnp.bfloat16)
    mix_out = product(mixed_heads, w_out)
    residual = (tokens.astype(jnp.float32) + mix_out).astype(jnp.bfloat16)
    ffn_in = row_norm(residual, ffn_gain).astype(jnp.bfloat16)
    route_share = route_weights / lax.optimization_barrier(jnp.sum(route_weights, axis=1, keepdims=True))
    rows_most = N_EP * CAP
    row_order = jnp.arange(seq_count, dtype=jnp.int32)
    zero_index = jnp.zeros((), jnp.int32)

    def one_expert(running, expert):
        hit_mask = route_ids == expert
        weight = lax.optimization_barrier(jnp.sum(jnp.where(hit_mask, route_share, 0.0), axis=1))
        taken_rows = jnp.any(hit_mask, axis=1)
        rank_key = jnp.where(taken_rows, 0, seq_count).astype(jnp.int32) + row_order
        picked = jnp.argsort(rank_key)[:rows_most].astype(jnp.int32)
        chosen_rows = ffn_in[picked]
        set_index = (expert // EXP_IN).astype(jnp.int32)
        sub_start = (expert % EXP_IN * FE).astype(jnp.int32)
        gate_block = lax.dynamic_slice(expert_gate, (set_index, zero_index, sub_start), (1, D, FE))[0]
        up_block = lax.dynamic_slice(expert_up, (set_index, zero_index, sub_start), (1, D, FE))[0]
        down_block = lax.dynamic_slice(expert_down, (set_index, sub_start, zero_index), (1, FE, D))[0]
        hidden = (jax.nn.silu(product(chosen_rows, gate_block)) * product(chosen_rows, up_block)).astype(jnp.bfloat16)
        result = product(hidden, down_block)
        running = running.at[picked].add(weight[picked][:, None] * result)
        return (running, None)
    moe_sum, unused = lax.scan(one_expert, jnp.zeros((seq_count, D), jnp.float32), jnp.arange(EXPERTS, dtype=jnp.int32))
    return (residual.astype(jnp.float32) + moe_sum).astype(jnp.bfloat16)
```

```python
import functools

import jax
import jax.numpy as jnp
from jax import lax
from jax.experimental import pallas as pl
from jax.experimental.pallas import tpu as pltpu
from jax.sharding import PartitionSpec as P

MESH = pl.DeviceIdType.MESH
NX = 4
HEAD_DIM = 64
STATE = 128
GROUPS = 2
EXP_IN = 4
EPS = 1e-06
F32 = jnp.float32
BF16 = jnp.bfloat16


def far_first(i, n):
    half = (i + 1) // 2
    return n // 2 + half * (1 - 2 * (i % 2))


def silu(v):
    return v / (1.0 + jnp.exp(-v))


def dot(a, b):
    return lax.dot_general(a, b, (((1,), (0,)), ((), ())), preferred_element_type=F32)


def dot_nt(a, b):
    return lax.dot_general(a, b, (((1,), (1,)), ((), ())), preferred_element_type=F32)


def kernel(ne, nt, nx, rows, *refs):
    (
        tokens, mix_gain, w_gate, w_value, w_key, w_query, w_step, step_bias, decay_log, skip_gain,
        conv_x, conv_b, conv_c, window_x, window_b, window_c, state, head_gain, w_out, ffn_gain,
        route_ids, route_weights, e_gate, e_up, e_down,
        out_ref,
        tok_v, mg_v, wgv_v, wkq_v, bias_v, dlog_v, skip_v, cx_v, cb_v, cc_v, wx_v, wb_v, wc_v,
        st_v, hg_v, wo_v, fg_v, ids_v, rw_v, eg_v, eu_v, ed_v,
        s1, g1, s2, r2, s3f, s3, r3, r3f, s4, g4, s5, r5, s6f, s6, r6,
        nbuf, part, sh_v, sl_v, pt_v, pk_v,
        load_sem, send_sem, recv_sem,
    ) = refs
    ep = lax.axis_index("ep")
    tp = lax.axis_index("tp")
    ny = nt // nx
    half = rows // 2
    width = nt * HEAD_DIM
    experts = EXP_IN * ne
    share_tp = nt // EXP_IN
    group = tp // (nt // GROUPS)
    gcol = pl.multiple_of(group * STATE, STATE)

    def tp_peer(i):
        y = (tp // nx + far_first(i // nx, ny)) % ny
        x = (tp % nx + far_first(i % nx, nx)) % nx
        return y * nx + x

    def ep_peer(i):
        z = (ep // 2 + far_first(i // 2, ne // 2)) % (ne // 2)
        return z * 2 + (ep % 2 + 1 - i % 2) % 2

    loads = []

    def load(src, dst):
        copy = pltpu.make_async_copy(src, dst, load_sem.at[len(loads)])
        copy.start()
        loads.append(copy)
        return copy

    load_tok = load(tokens, tok_v)
    barrier = pltpu.get_barrier_semaphore()

    def greet_tp(i, c):
        pl.semaphore_signal(barrier, inc=1, device_id={"tp": tp_peer(i)}, device_id_type=MESH)
        return c

    def greet_ep(i, c):
        pl.semaphore_signal(barrier, inc=1, device_id={"ep": ep_peer(i)}, device_id_type=MESH)
        return c

    lax.fori_loop(0, ne - 1, greet_ep, 0)
    lax.fori_loop(0, nt - 1, greet_tp, 0)

    load_ids = load(route_ids, ids_v)
    load_rw = load(route_weights, rw_v)
    load_state = load(state, st_v)
    load_win = [
        load(window_x, wx_v),
        load(window_b.at[:, :, pl.ds(gcol, STATE)], wb_v),
        load(window_c.at[:, :, pl.ds(gcol, STATE)], wc_v),
        load(conv_x, cx_v),
        load(conv_b.at[:, pl.ds(gcol, STATE)], cb_v),
        load(conv_c.at[:, pl.ds(gcol, STATE)], cc_v),
    ]
    load_mix = [
        load(mix_gain, mg_v),
        load(w_gate, wgv_v.at[pl.ds(0, HEAD_DIM)]),
        load(w_value, wgv_v.at[pl.ds(HEAD_DIM, HEAD_DIM)]),
        load(w_step, wgv_v.at[pl.ds(2 * HEAD_DIM, w_step.shape[0])]),
        load(w_key.at[:, pl.ds(gcol, STATE)], wkq_v.at[:, pl.ds(0, STATE)]),
        load(w_query.at[:, pl.ds(gcol, STATE)], wkq_v.at[:, pl.ds(STATE, STATE)]),
        load(step_bias, bias_v),
        load(decay_log, dlog_v),
        load(skip_gain, skip_v),
        load(head_gain, hg_v),
        load(w_out, wo_v),
    ]
    load_ffn = [load(ffn_gain, fg_v), load(e_gate, eg_v), load(e_up, eu_v), load(e_down, ed_v)]

    low = lax.broadcasted_iota(jnp.int32, (1, 2 * HEAD_DIM), 1) < HEAD_DIM

    def swap(a):
        return pltpu.roll(a, HEAD_DIM, 1)

    def unpack(a, b):
        top = jnp.where(low, a, swap(b))
        bottom = jnp.where(low, swap(a), b)
        return jnp.concatenate([top, bottom], axis=0)

    def pack(block):
        n = block.shape[0] // 2
        top, bottom = block[:n], block[n:]
        return jnp.where(low, top, swap(bottom)), jnp.where(low, swap(top), bottom)

    def exchange(phase, axis, peer_of, count, source, target, me):
        def send(i, c):
            peer = peer_of(i)
            pltpu.make_async_remote_copy(
                src_ref=source(peer),
                dst_ref=target.at[me],
                send_sem=send_sem.at[phase],
                recv_sem=recv_sem.at[phase],
                device_id={axis: peer},
                device_id_type=MESH,
            ).start()
            return c

        lax.fori_loop(0, count - 1, send, 0)

    def landed(phase, target, count, sem):
        some = target.at[pl.ds(0, count - 1)]
        pltpu.make_async_copy(some, some, sem.at[phase]).wait()

    load_tok.wait()
    tok = tok_v[...].astype(F32)
    tok_packed = jnp.concatenate([tok[:half], tok[half:]], axis=1)
    s1[...] = tok_packed.astype(BF16)
    g1[tp] = tok_packed.astype(BF16)
    pl.semaphore_wait(barrier, ne - 1 + nt - 1)
    exchange(0, "tp", tp_peer, nt, lambda peer: s1, g1, tp)

    load_ids.wait()
    load_rw.wait()
    line = lax.broadcasted_iota(jnp.int32, (experts, rows), 0)
    expert_of = (line % ne) * EXP_IN + line // ne
    ids = ids_v[...]
    hit = [(ids[k : k + 1] == expert_of).astype(F32) for k in range(2)]
    named = (hit[0] + hit[1]).astype(BF16)
    before = (
        lax.broadcasted_iota(jnp.int32, (rows, rows), 0) < lax.broadcasted_iota(jnp.int32, (rows, rows), 1)
    ).astype(BF16)
    earlier = dot(named, before)
    rank = [(earlier < 0.5).astype(F32), (earlier > 0.5).astype(F32)]
    for r in range(2):
        pt_v[:, r * rows : (r + 1) * rows] = (named.astype(F32) * rank[r]).astype(BF16)
    for k in range(2):
        for r in range(2):
            pk_v[k * rows : (k + 1) * rows, r * experts : (r + 1) * experts] = (
                jnp.transpose(hit[k] * rank[r]).astype(BF16)
            )
    rw = rw_v[...]
    share = rw / jnp.sum(rw, axis=0, keepdims=True)
    eye = (
        lax.broadcasted_iota(jnp.int32, (rows, rows), 0) == lax.broadcasted_iota(jnp.int32, (rows, rows), 1)
    )
    share_col = [
        jnp.sum(jnp.where(eye, share[k : k + 1], 0.0), axis=1, keepdims=True) for k in range(2)
    ]
    load_state.wait()
    st = st_v[...]
    st_high = st.astype(BF16)
    sh_v[...] = st_high
    sl_v[...] = (st - st_high.astype(F32)).astype(BF16)
    for copy in load_win:
        copy.wait()

    def taps(window, weight):
        w = weight[...].astype(F32)
        total = window[0].astype(F32) * w[0:1]
        for j in range(1, 3):
            total = total + window[j].astype(F32) * w[j : j + 1]
        return total, w[3:4]

    past_x, tap_x = taps(wx_v, cx_v)
    past_b, tap_b = taps(wb_v, cb_v)
    past_c, tap_c = taps(wc_v, cc_v)
    for copy in load_mix:
        copy.wait()
    mine = lax.broadcasted_iota(jnp.int32, (1, nt), 1) == tp

    def head_scalar(ref):
        return jnp.sum(jnp.where(mine, ref[...], 0.0), axis=1, keepdims=True)

    bias = head_scalar(bias_v)
    decay_rate = jnp.exp(head_scalar(dlog_v))
    skip = head_scalar(skip_v)

    landed(0, g1, nt, recv_sem)
    blocks = []
    square = jnp.zeros((rows, 2 * HEAD_DIM), F32)
    for i in range(nt // 2):
        block = unpack(g1[2 * i].astype(F32), g1[2 * i + 1].astype(F32))
        square = square + block * block
        blocks.append(block)
    scale = lax.rsqrt(jnp.sum(square, axis=1, keepdims=True) / width + EPS)
    for i, block in enumerate(blocks):
        cols = slice(128 * i, 128 * i + 128)
        nbuf[:, cols] = (block * scale * mg_v[:, cols]).astype(BF16)
    normed = nbuf[...]
    kq = dot(normed, wkq_v[...])
    gvs = dot_nt(normed, wgv_v[...])
    gate_z = gvs[:, :HEAD_DIM]
    raw_v = gvs[:, HEAD_DIM : 2 * HEAD_DIM]
    keys = silu(past_b + kq[:, :STATE] * tap_b)
    queries = silu(past_c + kq[:, STATE:] * tap_c)
    values = silu(past_x + raw_v * tap_x)
    step_in = jnp.sum(jnp.where(mine, gvs[:, 2 * HEAD_DIM :], 0.0), axis=1, keepdims=True) + bias
    step = jnp.maximum(step_in, 0.0) + jnp.log1p(jnp.exp(-jnp.abs(step_in)))
    decay = jnp.exp(-step * decay_rate)
    key_query = jnp.sum(keys * queries, axis=1, keepdims=True)
    q_high = queries.astype(BF16)
    q_low = (queries - q_high.astype(F32)).astype(BF16)
    pieces = []
    unit = min(8, rows)
    for g in range(rows // unit):
        seqs = slice(g * unit, (g + 1) * unit)
        lines = slice(g * unit * HEAD_DIM, (g + 1) * unit * HEAD_DIM)
        high = sh_v[lines]
        prod = dot_nt(q_high[seqs], high) + dot_nt(q_low[seqs], high) + dot_nt(q_high[seqs], sl_v[lines])
        row = lax.broadcasted_iota(jnp.int32, (unit, 2 * HEAD_DIM), 0)
        lane = lax.broadcasted_iota(jnp.int32, (unit, 2 * HEAD_DIM), 1)
        total = jnp.zeros((unit, 2 * HEAD_DIM), F32)
        for j in range(unit // 2):
            own = row == 2 * j + lane // HEAD_DIM
            total = total + jnp.where(own, prod[:, 128 * j : 128 * j + 128], 0.0)
        pieces.append((total + swap(total))[:, :HEAD_DIM])
    state_query = jnp.concatenate(pieces, axis=0)
    read_out = decay * state_query + (step * key_query + skip) * values
    gated = read_out * silu(gate_z)
    gated = gated * lax.rsqrt(jnp.mean(gated * gated, axis=1, keepdims=True) + EPS)
    mixed = (gated * hg_v[...]).astype(BF16)
    part[:rows, :] = dot(mixed, wo_v[...])
    for i in range(nt // 2):
        a, b = pack(part[:rows, 128 * i : 128 * i + 128])
        s2[2 * i] = a.astype(BF16)
        s2[2 * i + 1] = b.astype(BF16)
    exchange(1, "tp", tp_peer, nt, lambda peer: s2.at[peer], r2, tp)
    r2[tp] = s2[tp]
    landed(1, r2, nt, recv_sem)
    summed = r2[0].astype(F32)
    for i in range(1, nt):
        summed = summed + r2[i].astype(F32)
    residual = (tok_packed + summed).astype(BF16).astype(F32)

    turned = swap(residual)
    placed = jnp.concatenate(
        [
            jnp.where(low, residual, 0.0),
            jnp.where(low, turned, 0.0),
            jnp.where(low, 0.0, turned),
            jnp.where(low, 0.0, residual),
        ],
        axis=0,
    ).astype(BF16)
    slots = dot(pt_v[...], placed)
    for q in range(EXP_IN):
        s3f[:, q, :] = slots[q * ne : (q + 1) * ne]
    s3[...] = s3f[...].astype(BF16)
    exchange(2, "ep", ep_peer, ne, lambda peer: s3.at[peer], r3, ep)
    r3[ep] = s3[ep]
    landed(2, r3, ne, recv_sem)

    r3f[...] = r3[...].astype(F32)
    for q in range(EXP_IN):
        s4[q] = r3f[:, q, :].astype(BF16)
    exchange(3, "tp", tp_peer, nt, lambda peer: s4.at[peer // share_tp], g4, tp)
    g4[tp] = s4[tp // share_tp]
    for copy in load_ffn:
        copy.wait()
    landed(3, g4, nt, recv_sem)
    blocks = []
    square = jnp.zeros((2 * ne, 2 * HEAD_DIM), F32)
    for i in range(nt // 2):
        block = unpack(g4[2 * i].astype(F32), g4[2 * i + 1].astype(F32))
        square = square + block * block
        blocks.append(block)
    scale = lax.rsqrt(jnp.sum(square, axis=1, keepdims=True) / width + EPS)
    for i, block in enumerate(blocks):
        cols = slice(128 * i, 128 * i + 128)
        part[: 2 * ne, cols] = block * scale * fg_v[:, cols]
    ffn_in = part[: 2 * ne, :].astype(BF16)
    hidden = (silu(dot(ffn_in, eg_v[...])) * dot(ffn_in, eu_v[...])).astype(BF16)
    part[: 2 * ne, :] = dot(hidden, ed_v[...])
    for i in range(nt // 2):
        a, b = pack(part[: 2 * ne, 128 * i : 128 * i + 128])
        s5[2 * i] = a.astype(BF16)
        s5[2 * i + 1] = b.astype(BF16)
    exchange(4, "tp", tp_peer, nt, lambda peer: s5.at[peer], r5, tp)
    r5[tp] = s5[tp]
    landed(4, r5, nt, recv_sem)
    for q in range(EXP_IN):
        total = r5[q * share_tp].astype(F32)
        for i in range(1, share_tp):
            total = total + r5[q * share_tp + i].astype(F32)
        s6f[:, q, :] = total
    s6[...] = s6f[...].astype(BF16)
    exchange(5, "ep", ep_peer, ne, lambda peer: s6.at[peer], r6, ep)
    r6[ep] = s6[ep]
    landed(5, r6, ne, recv_sem)
    r3f[...] = r6[...].astype(F32)
    back = jnp.concatenate([r3f[:, q, :] for q in range(EXP_IN)], axis=0)
    back = jnp.concatenate([back, swap(back)], axis=0).astype(BF16)
    each = dot(pk_v[...], back)
    moe = share_col[0] * each[:rows] + share_col[1] * each[rows:]
    plain = jnp.concatenate([residual, swap(residual)], axis=0)
    out_ref[...] = (plain + moe)[:, :HEAD_DIM].astype(BF16)

    for phase, (ref, count) in enumerate(((g1, nt), (s2, nt), (s3, ne), (g4, nt), (s5, nt), (s6, ne))):
        landed(phase, ref, count, send_sem)


def local(nx, *args):
    (
        tokens, mix_gain, w_gate, w_value, w_key, w_query, w_step, step_bias, decay_log, skip_gain,
        conv_x, conv_b, conv_c, window_x, window_b, window_c, state, head_gain, w_out, ffn_gain,
        route_ids, route_weights, e_gate, e_up, e_down,
    ) = args
    ne, nt = lax.axis_size("ep"), lax.axis_size("tp")
    rows = tokens.shape[0]
    half = rows // 2
    width = nt * HEAD_DIM
    experts = EXP_IN * ne
    operands = (
        tokens, mix_gain[None], w_gate.T, w_value.T, w_key, w_query, w_step.T,
        step_bias[None], decay_log[None], skip_gain[None],
        conv_x, conv_b, conv_c,
        window_x.transpose(1, 0, 2), window_b.transpose(1, 0, 2), window_c.transpose(1, 0, 2),
        state.reshape(rows * HEAD_DIM, STATE), head_gain[None], w_out, ffn_gain[None],
        route_ids.T, route_weights.T, e_gate[0], e_up[0], e_down[0],
    )
    tall = max(rows, 2 * ne)
    hidden = e_gate.shape[2]
    vmem = pltpu.VMEM
    scratch = [
        vmem((rows, HEAD_DIM), BF16), vmem((1, width), F32), vmem((2 * HEAD_DIM + nt, width), BF16),
        vmem((width, 2 * STATE), BF16), vmem((1, nt), F32), vmem((1, nt), F32), vmem((1, nt), F32),
        vmem((4, HEAD_DIM), BF16), vmem((4, STATE), BF16), vmem((4, STATE), BF16),
        vmem((3, rows, HEAD_DIM), BF16), vmem((3, rows, STATE), BF16), vmem((3, rows, STATE), BF16),
        vmem((rows * HEAD_DIM, STATE), F32), vmem((1, HEAD_DIM), F32), vmem((HEAD_DIM, width), BF16),
        vmem((1, width), F32), vmem((2, rows), jnp.int32), vmem((2, rows), F32),
        vmem((width, hidden), BF16), vmem((width, hidden), BF16), vmem((hidden, width), BF16),
        vmem((half, 128), BF16), vmem((nt, half, 128), BF16),
        vmem((nt, half, 128), BF16), vmem((nt, half, 128), BF16),
        vmem((ne, EXP_IN, 128), F32), vmem((ne, EXP_IN, 128), BF16), vmem((ne, EXP_IN, 128), BF16),
        vmem((ne, EXP_IN, 128), F32),
        vmem((EXP_IN, ne, 128), BF16), vmem((nt, ne, 128), BF16),
        vmem((nt, ne, 128), BF16), vmem((nt, ne, 128), BF16),
        vmem((ne, EXP_IN, 128), F32), vmem((ne, EXP_IN, 128), BF16), vmem((ne, EXP_IN, 128), BF16),
        vmem((rows, width), BF16), vmem((tall, width), F32),
        vmem((rows * HEAD_DIM, STATE), BF16), vmem((rows * HEAD_DIM, STATE), BF16),
        vmem((experts, 2 * rows), BF16), vmem((2 * rows, 2 * experts), BF16),
        pltpu.SemaphoreType.DMA((25,)), pltpu.SemaphoreType.DMA((6,)), pltpu.SemaphoreType.DMA((6,)),
    ]
    return pl.pallas_call(
        functools.partial(kernel, ne, nt, nx, rows),
        out_shape=jax.ShapeDtypeStruct((rows, HEAD_DIM), BF16),
        in_specs=[pl.BlockSpec(memory_space=pl.ANY)] * len(operands),
        out_specs=pl.BlockSpec(memory_space=pltpu.VMEM),
        scratch_shapes=scratch,
        compiler_params=pltpu.CompilerParams(
            collective_id=0, has_side_effects=True
        ),
    )(*operands)


def solution(mesh):
    in_specs = (
        P("ep", "tp"), P(), P(None, "tp"), P(None, "tp"), P(), P(), P(), P(), P(), P(),
        P(None, "tp"), P(), P(), P("ep", None, "tp"), P("ep", None, None), P("ep", None, None),
        P("ep", "tp", None, None), P("tp"), P("tp", None), P(), P("ep", None), P("ep", None),
        P("ep", None, "tp"), P("ep", None, "tp"), P("ep", "tp", None),
    )
    return jax.shard_map(
        functools.partial(local, NX), mesh=mesh, in_specs=in_specs, out_specs=P("ep", "tp"), check_vma=False
    )
```

```python
import functools

import jax
import jax.numpy as jnp
from jax import lax
from jax.experimental import pallas as pl
from jax.experimental.pallas import tpu as pltpu
from jax.sharding import PartitionSpec as P

MESH = pl.DeviceIdType.MESH
NX = 4
HEAD_DIM = 64
STATE = 128
GROUPS = 2
EXP_IN = 4
EPS = 1e-06
F32 = jnp.float32
BF16 = jnp.bfloat16


def far_first(i, n):
    half = lax.div(i + 1, 2)
    return n // 2 + half * (1 - 2 * lax.rem(i, 2))


def silu(v):
    return v / (1.0 + jnp.exp(-v))


def dot(a, b):
    return lax.dot_general(a, b, (((1,), (0,)), ((), ())), preferred_element_type=F32)


def dot_nt(a, b):
    return lax.dot_general(a, b, (((1,), (1,)), ((), ())), preferred_element_type=F32)


def kernel(ne, nt, nx, rows, *refs):
    (
        tokens, mix_gain, w_gate, w_value, w_key, w_query, w_step, step_bias, decay_log, skip_gain,
        conv_x, conv_b, conv_c, window_x, window_b, window_c, state, head_gain, w_out, ffn_gain,
        route_ids, route_weights, e_gate, e_up, e_down,
        out_ref,
        tok_v, mg_v, wgv_v, wall_v, bias_v, dlog_v, skip_v, cx_v, cb_v, cc_v, wx_v, wb_v, wc_v,
        st_v, hg_v, wo_v, fg_v, ids_v, rw_v, egu_v, ed_v,
        s1, g1, s2, r2, s3f, s3, r3, r3f, s4, g4, s5, r5, s6f, s6, r6,
        xbuf, nbuf, sh_v, sl_v, pt_v, pk_v,
        load_sem, send_sem, row_sem, recv_sem, near_sem, far_sem, all_sem,
    ) = refs
    ep = lax.axis_index("ep")
    tp = lax.axis_index("tp")
    ny, nz = nt // nx, ne // 2
    half = rows // 2
    eh = ne // 2
    width = nt * HEAD_DIM
    span = nx * HEAD_DIM
    experts = EXP_IN * ne
    share_tp = nt // EXP_IN
    group = tp // (nt // GROUPS)
    gcol = pl.multiple_of(group * STATE, STATE)
    ty, tx = lax.div(tp, nx), lax.rem(tp, nx)
    ez, ec = lax.div(ep, 2), lax.rem(ep, 2)
    my_half = lax.div(ep, eh)
    offsets = [nx // 2 + ((i + 1) // 2) * (1 - 2 * (i % 2)) for i in range(nx)]
    xs = [lax.rem(tx + d, nx) for d in offsets]

    def for_rows(body):
        def step(i, c):
            body(lax.rem(ty + far_first(i, ny), ny), xs)
            return c

        lax.fori_loop(0, ny - 1, step, 0)
        body(ty, xs[:-1])

    def for_sets(body):
        def step(i, c):
            z = lax.rem(ez + far_first(i, nz), nz)
            body(2 * z + 1 - ec)
            body(2 * z + ec)
            return c

        lax.fori_loop(0, nz - 1, step, 0)
        body(2 * ez + 1 - ec)

    loads = []

    def load(src, dst):
        copy = pltpu.make_async_copy(src, dst, load_sem.at[len(loads)])
        copy.start()
        loads.append(copy)
        return copy

    load_tok = load(tokens, tok_v)
    barrier = pltpu.get_barrier_semaphore()

    def greet(axis, peer):
        pl.semaphore_signal(barrier, inc=1, device_id={axis: peer}, device_id_type=MESH)

    def inside(d):
        return jnp.logical_and(ez + d >= 0, ez + d < nz)

    def reach(*steps):
        return sum(inside(d).astype(jnp.int32) for d in steps)

    def tell(sem, *steps):
        for d in steps:
            @pl.when(inside(d))
            def _():
                pl.semaphore_signal(sem, inc=1, device_id={"ep": ep + 2 * d}, device_id_type=MESH)

    for d in (2, -2, 1, -1):
        @pl.when(inside(d))
        def _():
            for c in range(2):
                greet("ep", 2 * (ez + d) + c)

    greet("ep", 2 * ez + 1 - ec)

    def greet_row(y, cols):
        for x in cols:
            greet("tp", y * nx + x)

    for_rows(greet_row)

    load_ids = load(route_ids, ids_v)
    load_rw = load(route_weights, rw_v)
    load_state = load(state, st_v)
    load_win = [
        load(window_x, wx_v),
        load(window_b.at[:, :, pl.ds(gcol, STATE)], wb_v),
        load(window_c.at[:, :, pl.ds(gcol, STATE)], wc_v),
        load(conv_x, cx_v),
        load(conv_b.at[:, pl.ds(gcol, STATE)], cb_v),
        load(conv_c.at[:, pl.ds(gcol, STATE)], cc_v),
    ]
    load_mix = [
        load(mix_gain, mg_v),
        load(w_gate, wgv_v.at[pl.ds(0, HEAD_DIM)]),
        load(w_value, wgv_v.at[pl.ds(HEAD_DIM, HEAD_DIM)]),
        load(w_step, wgv_v.at[pl.ds(2 * HEAD_DIM, w_step.shape[0])]),
        load(w_key.at[:, pl.ds(gcol, STATE)], wall_v.at[:, pl.ds(0, STATE)]),
        load(w_query.at[:, pl.ds(gcol, STATE)], wall_v.at[:, pl.ds(STATE, STATE)]),
        load(step_bias, bias_v),
        load(decay_log, dlog_v),
        load(skip_gain, skip_v),
        load(head_gain, hg_v),
        load(w_out, wo_v),
    ]
    hidden_w = e_gate.shape[1]
    load_ffn = [
        load(ffn_gain, fg_v),
        load(e_gate, egu_v.at[:, pl.ds(0, hidden_w)]),
        load(e_up, egu_v.at[:, pl.ds(hidden_w, hidden_w)]),
        load(e_down, ed_v),
    ]

    low = lax.broadcasted_iota(jnp.int32, (1, 2 * HEAD_DIM), 1) < HEAD_DIM

    def swap(a):
        return pltpu.roll(a, HEAD_DIM, 1)

    def unpack(a, b):
        top = jnp.where(low, a, swap(b))
        bottom = jnp.where(low, swap(a), b)
        return jnp.concatenate([top, bottom], axis=0)

    def pack(block):
        n = block.shape[0] // 2
        top, bottom = block[:n], block[n:]
        return jnp.where(low, top, swap(bottom)), jnp.where(low, swap(top), bottom)

    def send_row(phase, y, cols, source, slot, sem):
        for x in cols:
            peer = y * nx + x
            pltpu.make_async_remote_copy(
                src_ref=source(peer),
                dst_ref=slot,
                send_sem=send_sem.at[phase],
                recv_sem=sem,
                device_id={"tp": peer},
                device_id_type=MESH,
            ).start()

    def send_set(phase, peer, source, slot, sem):
        pltpu.make_async_remote_copy(
            src_ref=source,
            dst_ref=slot,
            send_sem=send_sem.at[phase],
            recv_sem=sem,
            device_id={"ep": peer},
            device_id_type=MESH,
        ).start()

    def arrive(ref, sem):
        pltpu.make_async_copy(ref, ref, sem).wait()

    def rows_arrived(phase, target, start, use):
        arrive(target.at[pl.ds(0, nx - 1)], row_sem.at[phase, ty])
        carry = use(ty, start)

        def step(i, c):
            y = lax.rem(ty + far_first(ny - 2 - i, ny), ny)
            arrive(target.at[pl.ds(0, nx)], row_sem.at[phase, y])
            return use(y, c)

        return lax.fori_loop(0, ny - 1, step, carry)

    def spread_row(target, y, square):
        for j in range(nx // 2):
            block = unpack(target[y * nx + 2 * j].astype(F32), target[y * nx + 2 * j + 1].astype(F32))
            square = square + block * block
            col = y * span + 2 * HEAD_DIM * j
            if not isinstance(y, int):
                col = pl.multiple_of(col, 2 * HEAD_DIM)
            xbuf[: block.shape[0], pl.ds(col, 2 * HEAD_DIM)] = block
        return square

    def normalized(n, square, gain):
        scale = lax.rsqrt(jnp.sum(square, axis=1, keepdims=True) / width + EPS)
        for i in range(nt // 2):
            cols = slice(128 * i, 128 * i + 128)
            nbuf[:n, cols] = (xbuf[:n, cols] * scale * gain[:, cols]).astype(BF16)
        return nbuf[:n, :]

    load_tok.wait()
    tok = tok_v[...].astype(F32)
    tok_packed = jnp.concatenate([tok[:half], tok[half:]], axis=1)
    s1[...] = tok_packed.astype(BF16)
    g1[tp] = tok_packed.astype(BF16)
    pl.semaphore_wait(barrier, 2 * reach(2, -2, 1, -1) + nt)
    for_rows(lambda y, cols: send_row(0, y, cols, lambda peer: s1, g1.at[tp], row_sem.at[0, ty]))
    tell(near_sem, 2, -2)

    load_ids.wait()
    load_rw.wait()
    line = lax.broadcasted_iota(jnp.int32, (experts, rows), 0)
    expert_of = (line % ne) * EXP_IN + line // ne
    ids = ids_v[...]
    hit = [(ids[k : k + 1] == expert_of).astype(F32) for k in range(2)]
    named = (hit[0] + hit[1]).astype(BF16)
    before = (
        lax.broadcasted_iota(jnp.int32, (rows, rows), 0) < lax.broadcasted_iota(jnp.int32, (rows, rows), 1)
    ).astype(BF16)
    earlier = dot(named, before)
    rank = [(earlier < 0.5).astype(F32), (earlier > 0.5).astype(F32)]
    for r in range(2):
        pt_v[:, r * rows : (r + 1) * rows] = (named.astype(F32) * rank[r]).astype(BF16)
    for k in range(2):
        for r in range(2):
            pk_v[k * rows : (k + 1) * rows, r * experts : (r + 1) * experts] = (
                jnp.transpose(hit[k] * rank[r]).astype(BF16)
            )
    rw = rw_v[...]
    share = rw / jnp.sum(rw, axis=0, keepdims=True)
    eye = (
        lax.broadcasted_iota(jnp.int32, (rows, rows), 0) == lax.broadcasted_iota(jnp.int32, (rows, rows), 1)
    )
    share_col = [
        jnp.sum(jnp.where(eye, share[k : k + 1], 0.0), axis=1, keepdims=True) for k in range(2)
    ]
    load_state.wait()
    st = st_v[...]
    st_high = st.astype(BF16)
    sh_v[...] = st_high
    sl_v[...] = (st - st_high.astype(F32)).astype(BF16)
    for copy in load_win:
        copy.wait()

    def taps(window, weight):
        w = weight[...].astype(F32)
        total = window[0].astype(F32) * w[0:1]
        for j in range(1, 3):
            total = total + window[j].astype(F32) * w[j : j + 1]
        return total, w[3:4]

    past_x, tap_x = taps(wx_v, cx_v)
    past_b, tap_b = taps(wb_v, cb_v)
    past_c, tap_c = taps(wc_v, cc_v)
    for copy in load_mix:
        copy.wait()
    wall_v[:, 2 * STATE :] = jnp.transpose(wgv_v[...])
    mine = lax.broadcasted_iota(jnp.int32, (1, nt), 1) == tp

    def head_scalar(ref):
        return jnp.sum(jnp.where(mine, ref[...], 0.0), axis=1, keepdims=True)

    bias = head_scalar(bias_v)
    decay_rate = jnp.exp(head_scalar(dlog_v))
    skip = head_scalar(skip_v)

    pl.semaphore_wait(near_sem, reach(2, -2))
    tell(far_sem, 4, -4)
    def spread():
        pl.semaphore_wait(far_sem, reach(4, -4))
        pl.semaphore_signal(
            all_sem, inc=1, device_id={"ep": lax.rem(ep + eh, ne)}, device_id_type=MESH
        )

    pl.when(my_half == 1)(spread)

    square = rows_arrived(
        0, g1, jnp.zeros((rows, 2 * HEAD_DIM), F32), lambda y, c: spread_row(g1, y, c)
    )
    both = dot(normalized(rows, square, mg_v), wall_v[...])
    kq, gvs = both[:, : 2 * STATE], both[:, 2 * STATE :]
    gate_z = gvs[:, :HEAD_DIM]
    raw_v = gvs[:, HEAD_DIM : 2 * HEAD_DIM]
    keys = silu(past_b + kq[:, :STATE] * tap_b)
    queries = silu(past_c + kq[:, STATE:] * tap_c)
    values = silu(past_x + raw_v * tap_x)
    step_in = jnp.sum(jnp.where(mine, gvs[:, 2 * HEAD_DIM :], 0.0), axis=1, keepdims=True) + bias
    step = jnp.maximum(step_in, 0.0) + jnp.log1p(jnp.exp(-jnp.abs(step_in)))
    decay = jnp.exp(-step * decay_rate)
    key_query = jnp.sum(keys * queries, axis=1, keepdims=True)
    q_high = queries.astype(BF16)
    q_low = (queries - q_high.astype(F32)).astype(BF16)
    pieces = []
    unit = min(8, rows)
    for g in range(rows // unit):
        seqs = slice(g * unit, (g + 1) * unit)
        lines = slice(g * unit * HEAD_DIM, (g + 1) * unit * HEAD_DIM)
        both = jnp.concatenate([q_high[seqs].astype(F32), q_low[seqs].astype(F32)], axis=0).astype(BF16)
        prod = dot_nt(both, sh_v[lines])
        prod = prod[:unit] + prod[unit:] + dot_nt(q_high[seqs], sl_v[lines])
        row = lax.broadcasted_iota(jnp.int32, (unit, 2 * HEAD_DIM), 0)
        lane = lax.broadcasted_iota(jnp.int32, (unit, 2 * HEAD_DIM), 1)
        total = jnp.zeros((unit, 2 * HEAD_DIM), F32)
        for j in range(unit // 2):
            own = row == 2 * j + lane // HEAD_DIM
            total = total + jnp.where(own, prod[:, 128 * j : 128 * j + 128], 0.0)
        pieces.append((total + swap(total))[:, :HEAD_DIM])
    state_query = jnp.concatenate(pieces, axis=0)
    read_out = decay * state_query + (step * key_query + skip) * values
    gated = read_out * silu(gate_z)
    gated = gated * lax.rsqrt(jnp.mean(gated * gated, axis=1, keepdims=True) + EPS)
    mixed = (gated * hg_v[...]).astype(BF16)

    def packed_product(left, right, target):
        out = dot(left, right[...])
        for j in range(nt // 2):
            a, b = pack(out[:, 128 * j : 128 * j + 128])
            target[2 * j] = a.astype(BF16)
            target[2 * j + 1] = b.astype(BF16)

    packed_product(mixed, wo_v, s2)
    for_rows(lambda y, cols: send_row(1, y, cols, lambda peer: s2.at[peer], r2.at[tp], row_sem.at[1, ty]))
    r2[tp] = s2[tp]
    pl.when(my_half == 0)(spread)

    def add_row(y, total):
        for x in range(nx):
            total = total + r2[y * nx + x].astype(F32)
        return total

    summed = rows_arrived(1, r2, jnp.zeros((half, 2 * HEAD_DIM), F32), add_row)
    residual = (tok_packed + summed).astype(BF16).astype(F32)
    turned = swap(residual)
    placed = jnp.concatenate(
        [
            jnp.where(low, residual, 0.0),
            jnp.where(low, turned, 0.0),
            jnp.where(low, 0.0, turned),
            jnp.where(low, 0.0, residual),
        ],
        axis=0,
    ).astype(BF16)
    slots = dot(pt_v[...], placed)
    for q in range(EXP_IN):
        s3f[:, q, :] = slots[q * ne : (q + 1) * ne]
    s3[...] = s3f[...].astype(BF16)
    pl.semaphore_wait(all_sem, 1)
    for_sets(lambda peer: send_set(2, peer, s3.at[peer], r3.at[ep], recv_sem.at[my_half]))
    r3[ep] = s3[ep]

    def sets_arrived(h):
        @pl.when(my_half == h)
        def _():
            arrive(r3.at[pl.ds(0, eh - 1)], recv_sem.at[h])

        @pl.when(my_half != h)
        def _():
            arrive(r3.at[pl.ds(0, eh)], recv_sem.at[h])

    def gather_half(h):
        r3f[...] = r3[h * eh : (h + 1) * eh].astype(F32)
        for q in range(EXP_IN):
            s4[h, q] = r3f[:, q, :].astype(BF16)

        def row(y, cols):
            sub = lax.div(y * nx, share_tp)
            if share_tp < nx:
                send_row(3 + h, y, cols, lambda peer: s4.at[h, lax.div(peer, share_tp)], g4.at[h, tp], row_sem.at[2 + h, ty])
            else:
                send_row(3 + h, y, cols, lambda peer: s4.at[h, sub], g4.at[h, tp], row_sem.at[2 + h, ty])

        for_rows(row)
        g4[h, tp] = s4[h, lax.div(tp, share_tp)]

    def expert_half(h):
        square = rows_arrived(
            2 + h, g4.at[h], jnp.zeros((2 * eh, 2 * HEAD_DIM), F32), lambda y, c: spread_row(g4.at[h], y, c)
        )
        both = dot(normalized(2 * eh, square, fg_v), egu_v[...])
        hidden = (silu(both[:, :hidden_w]) * both[:, hidden_w:]).astype(BF16)

        packed_product(hidden, ed_v, s5.at[h])
        for_rows(
            lambda y, cols: send_row(
                5 + h, y, cols, lambda peer: s5.at[h, peer], r5.at[h, tp], recv_sem.at[2 + h]
            )
        )
        r5[h, tp] = s5[h, tp]

    def return_half(h):
        arrive(r5.at[h, pl.ds(0, nt - 1)], recv_sem.at[2 + h])
        for q in range(EXP_IN):
            total = r5[h, q * share_tp].astype(F32)
            for i in range(1, share_tp):
                total = total + r5[h, q * share_tp + i].astype(F32)
            s6f[:, q, :] = total
        s6[h * eh : (h + 1) * eh] = s6f[...].astype(BF16)

        def back(peer):
            @pl.when(lax.div(peer, eh) == h)
            def _():
                send_set(7, peer, s6.at[peer], r6.at[ep], recv_sem.at[4])

        for_sets(back)

    sets_arrived(0)
    gather_half(0)
    sets_arrived(1)
    gather_half(1)
    for copy in load_ffn:
        copy.wait()
    expert_half(0)
    expert_half(1)
    return_half(0)
    return_half(1)
    r6[ep] = s6[ep]
    arrive(r6.at[pl.ds(0, ne - 1)], recv_sem.at[4])
    s3f[...] = r6[...].astype(F32)
    back = jnp.concatenate([s3f[:, q, :] for q in range(EXP_IN)], axis=0)
    back = jnp.concatenate([back, swap(back)], axis=0).astype(BF16)
    each = dot(pk_v[...], back)
    moe = share_col[0] * each[:rows] + share_col[1] * each[rows:]
    plain = jnp.concatenate([residual, swap(residual)], axis=0)
    out_ref[...] = (plain + moe)[:, :HEAD_DIM]

    for phase, ref in enumerate(
        (
            g1.at[pl.ds(0, nt - 1)], s2.at[pl.ds(0, nt - 1)], s3.at[pl.ds(0, ne - 1)],
            g4.at[0, pl.ds(0, nt - 1)], g4.at[1, pl.ds(0, nt - 1)],
            s5.at[0, pl.ds(0, nt - 1)], s5.at[1, pl.ds(0, nt - 1)], s6.at[pl.ds(0, ne - 1)],
        )
    ):
        arrive(ref, send_sem.at[phase])


def local(nx, *args):
    (
        tokens, mix_gain, w_gate, w_value, w_key, w_query, w_step, step_bias, decay_log, skip_gain,
        conv_x, conv_b, conv_c, window_x, window_b, window_c, state, head_gain, w_out, ffn_gain,
        route_ids, route_weights, e_gate, e_up, e_down,
    ) = args
    ne, nt = lax.axis_size("ep"), lax.axis_size("tp")
    rows = tokens.shape[0]
    half = rows // 2
    width = nt * HEAD_DIM
    experts = EXP_IN * ne
    operands = (
        tokens, mix_gain[None], w_gate.T, w_value.T, w_key, w_query, w_step.T,
        step_bias[None], decay_log[None], skip_gain[None],
        conv_x, conv_b, conv_c,
        window_x.transpose(1, 0, 2), window_b.transpose(1, 0, 2), window_c.transpose(1, 0, 2),
        state.reshape(rows * HEAD_DIM, STATE), head_gain[None], w_out, ffn_gain[None],
        route_ids.T, route_weights.T, e_gate[0], e_up[0], e_down[0],
    )
    eh = ne // 2
    hidden = e_gate.shape[2]
    vmem = pltpu.VMEM
    scratch = [
        vmem((rows, HEAD_DIM), BF16), vmem((1, width), F32), vmem((2 * HEAD_DIM + nt, width), BF16),
        vmem((width, 2 * STATE + 2 * HEAD_DIM + nt), BF16), vmem((1, nt), F32), vmem((1, nt), F32), vmem((1, nt), F32),
        vmem((4, HEAD_DIM), BF16), vmem((4, STATE), BF16), vmem((4, STATE), BF16),
        vmem((3, rows, HEAD_DIM), BF16), vmem((3, rows, STATE), BF16), vmem((3, rows, STATE), BF16),
        vmem((rows * HEAD_DIM, STATE), F32), vmem((1, HEAD_DIM), F32), vmem((HEAD_DIM, width), BF16),
        vmem((1, width), F32), vmem((2, rows), jnp.int32), vmem((2, rows), F32),
        vmem((width, 2 * hidden), BF16), vmem((hidden, width), BF16),
        vmem((half, 128), BF16), vmem((nt, half, 128), BF16),
        vmem((nt, half, 128), BF16), vmem((nt, half, 128), BF16),
        vmem((ne, EXP_IN, 128), F32), vmem((ne, EXP_IN, 128), BF16), vmem((ne, EXP_IN, 128), BF16),
        vmem((eh, EXP_IN, 128), F32),
        vmem((2, EXP_IN, eh, 128), BF16), vmem((2, nt, eh, 128), BF16),
        vmem((2, nt, eh, 128), BF16), vmem((2, nt, eh, 128), BF16),
        vmem((eh, EXP_IN, 128), F32), vmem((ne, EXP_IN, 128), BF16), vmem((ne, EXP_IN, 128), BF16),
        vmem((max(rows, 2 * eh), width), F32), vmem((max(rows, 2 * eh), width), BF16),
        vmem((rows * HEAD_DIM, STATE), BF16), vmem((rows * HEAD_DIM, STATE), BF16),
        vmem((experts, 2 * rows), BF16), vmem((2 * rows, 2 * experts), BF16),
        pltpu.SemaphoreType.DMA((25,)), pltpu.SemaphoreType.DMA((8,)),
        pltpu.SemaphoreType.DMA((4, nt // nx)), pltpu.SemaphoreType.DMA((5,)),
        pltpu.SemaphoreType.REGULAR, pltpu.SemaphoreType.REGULAR, pltpu.SemaphoreType.REGULAR,
    ]
    total = pl.pallas_call(
        functools.partial(kernel, ne, nt, nx, rows),
        out_shape=jax.ShapeDtypeStruct((rows, HEAD_DIM), F32),
        in_specs=[pl.BlockSpec(memory_space=pl.ANY)] * len(operands),
        out_specs=pl.BlockSpec(memory_space=pltpu.VMEM),
        scratch_shapes=scratch,
        compiler_params=pltpu.CompilerParams(
            collective_id=0, has_side_effects=True
        ),
    )(*operands)
    return total.astype(BF16)


def solution(mesh):
    in_specs = (
        P("ep", "tp"), P(), P(None, "tp"), P(None, "tp"), P(), P(), P(), P(), P(), P(),
        P(None, "tp"), P(), P(), P("ep", None, "tp"), P("ep", None, None), P("ep", None, None),
        P("ep", "tp", None, None), P("tp"), P("tp", None), P(), P("ep", None), P("ep", None),
        P("ep", None, "tp"), P("ep", None, "tp"), P("ep", "tp", None),
    )
    return jax.shard_map(
        functools.partial(local, NX), mesh=mesh, in_specs=in_specs, out_specs=P("ep", "tp"), check_vma=False
    )
```

```python
import functools

import jax
import jax.numpy as jnp
from jax import lax
from jax.experimental import pallas as pl
from jax.experimental.pallas import tpu as pltpu
from jax.sharding import PartitionSpec as P

MESH = pl.DeviceIdType.MESH
NX = 4
HEAD_DIM = 64
STATE = 128
GROUPS = 2
EXP_IN = 4
EPS = 1e-06
F32 = jnp.float32
BF16 = jnp.bfloat16


def far_first(i, n):
    half = lax.div(i + 1, 2)
    return n // 2 + half * (1 - 2 * lax.rem(i, 2))


def silu(v):
    return v / (1.0 + jnp.exp(-v))


def dot(a, b):
    return lax.dot_general(a, b, (((1,), (0,)), ((), ())), preferred_element_type=F32)


def dot_nt(a, b):
    return lax.dot_general(a, b, (((1,), (1,)), ((), ())), preferred_element_type=F32)


def kernel(ne, nt, nx, rows, *refs):
    (
        tokens, mix_gain, w_gate, w_value, w_key, w_query, w_step, step_bias, decay_log, skip_gain,
        conv_x, conv_b, conv_c, window_x, window_b, window_c, state, head_gain, w_out, ffn_gain,
        route_ids, route_weights, e_gate, e_up, e_down,
        out_ref,
        tok_v, mg_v, wgv_v, wall_v, bias_v, dlog_v, skip_v, cx_v, cb_v, cc_v, wx_v, wb_v, wc_v,
        st_v, hg_v, wo_v, fg_v, ids_v, rw_v, egu_v, ed_v,
        s1, g1, s2, r2, s3f, s3, r3, r3f, s4, g4, s5, r5, s6f, s6, r6,
        xbuf, nbuf, sh_v, sl_v, pt_v, pk_v,
        load_sem, send_sem, row_sem, recv_sem, near_sem, far_sem, all_sem,
    ) = refs
    ep = lax.axis_index("ep")
    tp = lax.axis_index("tp")
    ny, nz = nt // nx, ne // 2
    half = rows // 2
    eh = ne // 2
    width = nt * HEAD_DIM
    span = nx * HEAD_DIM
    experts = EXP_IN * ne
    share_tp = nt // EXP_IN
    group = tp // (nt // GROUPS)
    gcol = pl.multiple_of(group * STATE, STATE)
    ty, tx = lax.div(tp, nx), lax.rem(tp, nx)
    ez, ec = lax.div(ep, 2), lax.rem(ep, 2)
    my_half = lax.div(ep, eh)
    offsets = [nx // 2 + ((i + 1) // 2) * (1 - 2 * (i % 2)) for i in range(nx)]
    xs = [lax.rem(tx + d, nx) for d in offsets]

    def for_rows(body):
        def step(i, c):
            body(lax.rem(ty + far_first(i, ny), ny), xs)
            return c

        lax.fori_loop(0, ny - 1, step, 0)
        body(ty, xs[:-1])

    def for_sets(body):
        def step(i, c):
            z = lax.rem(ez + far_first(i, nz), nz)
            body(2 * z + 1 - ec)
            body(2 * z + ec)
            return c

        lax.fori_loop(0, nz - 1, step, 0)
        body(2 * ez + 1 - ec)

    loads = []

    def load(src, dst):
        copy = pltpu.make_async_copy(src, dst, load_sem.at[len(loads)])
        copy.start()
        loads.append(copy)
        return copy

    load_tok = load(tokens, tok_v)
    barrier = pltpu.get_barrier_semaphore()

    def greet(axis, peer):
        pl.semaphore_signal(barrier, inc=1, device_id={axis: peer}, device_id_type=MESH)

    def inside(d):
        return jnp.logical_and(ez + d >= 0, ez + d < nz)

    def reach(*steps):
        return sum(inside(d).astype(jnp.int32) for d in steps)

    def tell(sem, *steps):
        for d in steps:
            @pl.when(inside(d))
            def _():
                pl.semaphore_signal(sem, inc=1, device_id={"ep": ep + 2 * d}, device_id_type=MESH)

    for d in (2, -2, 1, -1):
        @pl.when(inside(d))
        def _():
            for c in range(2):
                greet("ep", 2 * (ez + d) + c)

    greet("ep", 2 * ez + 1 - ec)

    def greet_row(y, cols):
        for x in cols:
            greet("tp", y * nx + x)

    for_rows(greet_row)

    load_ids = load(route_ids, ids_v)
    load_rw = load(route_weights, rw_v)
    load_state = load(state, st_v)
    load_win = [
        load(window_x, wx_v),
        load(window_b.at[:, :, pl.ds(gcol, STATE)], wb_v),
        load(window_c.at[:, :, pl.ds(gcol, STATE)], wc_v),
        load(conv_x, cx_v),
        load(conv_b.at[:, pl.ds(gcol, STATE)], cb_v),
        load(conv_c.at[:, pl.ds(gcol, STATE)], cc_v),
    ]
    load_mix = [
        load(mix_gain, mg_v),
        load(w_gate, wgv_v.at[pl.ds(0, HEAD_DIM)]),
        load(w_value, wgv_v.at[pl.ds(HEAD_DIM, HEAD_DIM)]),
        load(w_step, wgv_v.at[pl.ds(2 * HEAD_DIM, w_step.shape[0])]),
        load(w_key.at[:, pl.ds(gcol, STATE)], wall_v.at[:, pl.ds(0, STATE)]),
        load(w_query.at[:, pl.ds(gcol, STATE)], wall_v.at[:, pl.ds(STATE, STATE)]),
        load(step_bias, bias_v),
        load(decay_log, dlog_v),
        load(skip_gain, skip_v),
        load(head_gain, hg_v),
        load(w_out, wo_v),
    ]
    hidden_w = e_gate.shape[1]
    load_ffn = [
        load(ffn_gain, fg_v),
        load(e_gate, egu_v.at[:, pl.ds(0, hidden_w)]),
        load(e_up, egu_v.at[:, pl.ds(hidden_w, hidden_w)]),
        load(e_down, ed_v),
    ]

    low = lax.broadcasted_iota(jnp.int32, (1, 2 * HEAD_DIM), 1) < HEAD_DIM

    def swap(a):
        return pltpu.roll(a, HEAD_DIM, 1)

    def unpack(a, b):
        top = jnp.where(low, a, swap(b))
        bottom = jnp.where(low, swap(a), b)
        return jnp.concatenate([top, bottom], axis=0)

    def pack(block):
        n = block.shape[0] // 2
        top, bottom = block[:n], block[n:]
        return jnp.where(low, top, swap(bottom)), jnp.where(low, swap(top), bottom)

    def send_row(phase, y, cols, source, slot, sem):
        for x in cols:
            peer = y * nx + x
            pltpu.make_async_remote_copy(
                src_ref=source(peer),
                dst_ref=slot,
                send_sem=send_sem.at[phase],
                recv_sem=sem,
                device_id={"tp": peer},
                device_id_type=MESH,
            ).start()

    def send_set(phase, peer, source, slot, sem):
        pltpu.make_async_remote_copy(
            src_ref=source,
            dst_ref=slot,
            send_sem=send_sem.at[phase],
            recv_sem=sem,
            device_id={"ep": peer},
            device_id_type=MESH,
        ).start()

    def arrive(ref, sem):
        pltpu.make_async_copy(ref, ref, sem).wait()

    def rows_arrived(phase, target, start, use):
        arrive(target.at[pl.ds(0, nx - 1)], row_sem.at[phase, ty])
        carry = use(ty, start)

        def step(i, c):
            y = lax.rem(ty + far_first(ny - 2 - i, ny), ny)
            arrive(target.at[pl.ds(0, nx)], row_sem.at[phase, y])
            return use(y, c)

        return lax.fori_loop(0, ny - 1, step, carry)

    def spread_row(target, y, square):
        for j in range(nx // 2):
            block = unpack(target[y * nx + 2 * j].astype(F32), target[y * nx + 2 * j + 1].astype(F32))
            square = square + block * block
            col = y * span + 2 * HEAD_DIM * j
            if not isinstance(y, int):
                col = pl.multiple_of(col, 2 * HEAD_DIM)
            xbuf[: block.shape[0], pl.ds(col, 2 * HEAD_DIM)] = block
        return square

    def normalized(n, square, gain):
        scale = lax.rsqrt(jnp.sum(square, axis=1, keepdims=True) / width + EPS)
        for i in range(nt // 2):
            cols = slice(128 * i, 128 * i + 128)
            nbuf[:n, cols] = (xbuf[:n, cols] * scale * gain[:, cols]).astype(BF16)
        return nbuf[:n, :]

    load_tok.wait()
    tok = tok_v[...].astype(F32)
    tok_packed = jnp.concatenate([tok[:half], tok[half:]], axis=1)
    s1[...] = tok_packed.astype(BF16)
    g1[tp] = tok_packed.astype(BF16)
    pl.semaphore_wait(barrier, 2 * reach(2, -2, 1, -1) + nt)
    for_rows(lambda y, cols: send_row(0, y, cols, lambda peer: s1, g1.at[tp], row_sem.at[0, ty]))
    tell(near_sem, 2, -2)

    load_ids.wait()
    load_rw.wait()
    line = lax.broadcasted_iota(jnp.int32, (experts, rows), 0)
    expert_of = (line % ne) * EXP_IN + line // ne
    ids = ids_v[...]
    hit = [(ids[k : k + 1] == expert_of).astype(F32) for k in range(2)]
    named = (hit[0] + hit[1]).astype(BF16)
    before = (
        lax.broadcasted_iota(jnp.int32, (rows, rows), 0) < lax.broadcasted_iota(jnp.int32, (rows, rows), 1)
    ).astype(BF16)
    earlier = dot(named, before)
    rank = [(earlier < 0.5).astype(F32), (earlier > 0.5).astype(F32)]
    for r in range(2):
        pt_v[:, r * rows : (r + 1) * rows] = (named.astype(F32) * rank[r]).astype(BF16)
    for k in range(2):
        for r in range(2):
            pk_v[k * rows : (k + 1) * rows, r * experts : (r + 1) * experts] = (
                jnp.transpose(hit[k] * rank[r]).astype(BF16)
            )
    rw = rw_v[...]
    share = rw / jnp.sum(rw, axis=0, keepdims=True)
    eye = (
        lax.broadcasted_iota(jnp.int32, (rows, rows), 0) == lax.broadcasted_iota(jnp.int32, (rows, rows), 1)
    )
    share_col = [
        jnp.sum(jnp.where(eye, share[k : k + 1], 0.0), axis=1, keepdims=True) for k in range(2)
    ]
    load_state.wait()
    wide = rows * HEAD_DIM // 6
    for i in range(6):
        lines = slice(i * wide, (i + 1) * wide)
        st = jnp.transpose(st_v[lines])
        st_high = st.astype(BF16)
        sh_v[:, lines] = st_high
        sl_v[:, lines] = (st - st_high.astype(F32)).astype(BF16)
    for copy in load_win:
        copy.wait()

    def taps(window, weight):
        w = weight[...].astype(F32)
        total = window[0].astype(F32) * w[0:1]
        for j in range(1, 3):
            total = total + window[j].astype(F32) * w[j : j + 1]
        return total, w[3:4]

    past_x, tap_x = taps(wx_v, cx_v)
    past_b, tap_b = taps(wb_v, cb_v)
    past_c, tap_c = taps(wc_v, cc_v)
    for copy in load_mix:
        copy.wait()
    wall_v[:, 2 * STATE :] = jnp.transpose(wgv_v[...])
    mine = lax.broadcasted_iota(jnp.int32, (1, nt), 1) == tp

    def head_scalar(ref):
        return jnp.sum(jnp.where(mine, ref[...], 0.0), axis=1, keepdims=True)

    bias = head_scalar(bias_v)
    decay_rate = jnp.exp(head_scalar(dlog_v))
    skip = head_scalar(skip_v)

    pl.semaphore_wait(near_sem, reach(2, -2))
    tell(far_sem, 4, -4)
    def spread():
        pl.semaphore_wait(far_sem, reach(4, -4))
        pl.semaphore_signal(
            all_sem, inc=1, device_id={"ep": lax.rem(ep + eh, ne)}, device_id_type=MESH
        )

    pl.when(my_half == 1)(spread)

    square = rows_arrived(
        0, g1, jnp.zeros((rows, 2 * HEAD_DIM), F32), lambda y, c: spread_row(g1, y, c)
    )
    both = dot(normalized(rows, square, mg_v), wall_v[...])
    kq, gvs = both[:, : 2 * STATE], both[:, 2 * STATE :]
    gate_z = gvs[:, :HEAD_DIM]
    raw_v = gvs[:, HEAD_DIM : 2 * HEAD_DIM]
    keys = silu(past_b + kq[:, :STATE] * tap_b)
    queries = silu(past_c + kq[:, STATE:] * tap_c)
    values = silu(past_x + raw_v * tap_x)
    step_in = jnp.sum(jnp.where(mine, gvs[:, 2 * HEAD_DIM :], 0.0), axis=1, keepdims=True) + bias
    step = jnp.maximum(step_in, 0.0) + jnp.log1p(jnp.exp(-jnp.abs(step_in)))
    decay = jnp.exp(-step * decay_rate)
    key_query = jnp.sum(keys * queries, axis=1, keepdims=True)
    q_high = queries.astype(BF16)
    q_low = (queries - q_high.astype(F32)).astype(BF16)
    pieces = []
    unit = min(8, rows)
    for g in range(rows // unit):
        seqs = slice(g * unit, (g + 1) * unit)
        lines = slice(g * unit * HEAD_DIM, (g + 1) * unit * HEAD_DIM)
        both = jnp.concatenate([q_high[seqs].astype(F32), q_low[seqs].astype(F32)], axis=0).astype(BF16)
        prod = dot(both, sh_v[:, lines])
        prod = prod[:unit] + prod[unit:] + dot(q_high[seqs], sl_v[:, lines])
        row = lax.broadcasted_iota(jnp.int32, (unit, 2 * HEAD_DIM), 0)
        lane = lax.broadcasted_iota(jnp.int32, (unit, 2 * HEAD_DIM), 1)
        total = jnp.zeros((unit, 2 * HEAD_DIM), F32)
        for j in range(unit // 2):
            own = row == 2 * j + lane // HEAD_DIM
            total = total + jnp.where(own, prod[:, 128 * j : 128 * j + 128], 0.0)
        pieces.append((total + swap(total))[:, :HEAD_DIM])
    state_query = jnp.concatenate(pieces, axis=0)
    read_out = decay * state_query + (step * key_query + skip) * values
    gated = read_out * silu(gate_z)
    gated = gated * lax.rsqrt(jnp.mean(gated * gated, axis=1, keepdims=True) + EPS)
    mixed = (gated * hg_v[...]).astype(BF16)

    def packed_product(left, right, target):
        out = dot(left, right[...])
        for j in range(nt // 2):
            a, b = pack(out[:, 128 * j : 128 * j + 128])
            target[2 * j] = a.astype(BF16)
            target[2 * j + 1] = b.astype(BF16)

    packed_product(mixed, wo_v, s2)
    for_rows(lambda y, cols: send_row(1, y, cols, lambda peer: s2.at[peer], r2.at[tp], row_sem.at[1, ty]))
    r2[tp] = s2[tp]
    pl.when(my_half == 0)(spread)

    def add_row(y, total):
        for x in range(nx):
            total = total + r2[y * nx + x].astype(F32)
        return total

    summed = rows_arrived(1, r2, jnp.zeros((half, 2 * HEAD_DIM), F32), add_row)
    residual = (tok_packed + summed).astype(BF16).astype(F32)
    turned = swap(residual)
    placed = jnp.concatenate(
        [
            jnp.where(low, residual, 0.0),
            jnp.where(low, turned, 0.0),
            jnp.where(low, 0.0, turned),
            jnp.where(low, 0.0, residual),
        ],
        axis=0,
    ).astype(BF16)
    slots = dot(pt_v[...], placed)
    for q in range(EXP_IN):
        s3f[:, q, :] = slots[q * ne : (q + 1) * ne]
    s3[...] = s3f[...].astype(BF16)
    pl.semaphore_wait(all_sem, 1)
    for_sets(lambda peer: send_set(2, peer, s3.at[peer], r3.at[ep], recv_sem.at[my_half]))
    r3[ep] = s3[ep]

    def sets_arrived(h):
        @pl.when(my_half == h)
        def _():
            arrive(r3.at[pl.ds(0, eh - 1)], recv_sem.at[h])

        @pl.when(my_half != h)
        def _():
            arrive(r3.at[pl.ds(0, eh)], recv_sem.at[h])

    def gather_half(h):
        r3f[...] = r3[h * eh : (h + 1) * eh].astype(F32)
        for q in range(EXP_IN):
            s4[h, q] = r3f[:, q, :].astype(BF16)

        def row(y, cols):
            sub = lax.div(y * nx, share_tp)
            if share_tp < nx:
                send_row(3 + h, y, cols, lambda peer: s4.at[h, lax.div(peer, share_tp)], g4.at[h, tp], row_sem.at[2 + h, ty])
            else:
                send_row(3 + h, y, cols, lambda peer: s4.at[h, sub], g4.at[h, tp], row_sem.at[2 + h, ty])

        for_rows(row)
        g4[h, tp] = s4[h, lax.div(tp, share_tp)]

    def expert_half(h):
        square = rows_arrived(
            2 + h, g4.at[h], jnp.zeros((2 * eh, 2 * HEAD_DIM), F32), lambda y, c: spread_row(g4.at[h], y, c)
        )
        ffn_in = normalized(2 * eh, square, fg_v)
        both = dot(ffn_in, egu_v[...])
        hidden = (silu(both[:, :hidden_w]) * both[:, hidden_w:]).astype(BF16)

        packed_product(hidden, ed_v, s5.at[h])
        for_rows(
            lambda y, cols: send_row(
                5 + h, y, cols, lambda peer: s5.at[h, peer], r5.at[h, tp], recv_sem.at[2 + h]
            )
        )
        r5[h, tp] = s5[h, tp]

    def return_half(h):
        arrive(r5.at[h, pl.ds(0, nt - 1)], recv_sem.at[2 + h])
        for q in range(EXP_IN):
            total = r5[h, q * share_tp].astype(F32)
            for i in range(1, share_tp):
                total = total + r5[h, q * share_tp + i].astype(F32)
            s6f[:, q, :] = total
        s6[h * eh : (h + 1) * eh] = s6f[...].astype(BF16)

        away = my_half != h
        zh = nz // 2

        def back(peer):
            send_set(7, peer, s6.at[peer], r6.at[ep], recv_sem.at[4])

        def place(i):
            return h * zh + lax.rem(ez + far_first(i, zh) + (zh // 2) * away.astype(jnp.int32), zh)

        def step(i, c):
            z = place(i)
            back(2 * z + 1 - ec)
            back(2 * z + ec)
            return c

        lax.fori_loop(0, zh - 1, step, 0)
        z = place(zh - 1)
        back(2 * z + 1 - ec)
        pl.when(away)(lambda: back(2 * z + ec))

    sets_arrived(0)
    gather_half(0)
    sets_arrived(1)
    gather_half(1)
    for copy in load_ffn:
        copy.wait()
    expert_half(0)
    expert_half(1)
    return_half(0)
    return_half(1)
    r6[ep] = s6[ep]
    arrive(r6.at[pl.ds(0, ne - 1)], recv_sem.at[4])
    s3f[...] = r6[...].astype(F32)
    back = jnp.concatenate([s3f[:, q, :] for q in range(EXP_IN)], axis=0)
    back = jnp.concatenate([back, swap(back)], axis=0).astype(BF16)
    each = dot(pk_v[...], back)
    moe = share_col[0] * each[:rows] + share_col[1] * each[rows:]
    plain = jnp.concatenate([residual, swap(residual)], axis=0)
    out_ref[...] = (plain + moe)[:, :HEAD_DIM]

    for phase, ref in enumerate(
        (
            g1.at[pl.ds(0, nt - 1)], s2.at[pl.ds(0, nt - 1)], s3.at[pl.ds(0, ne - 1)],
            g4.at[0, pl.ds(0, nt - 1)], g4.at[1, pl.ds(0, nt - 1)],
            s5.at[0, pl.ds(0, nt - 1)], s5.at[1, pl.ds(0, nt - 1)], s6.at[pl.ds(0, ne - 1)],
        )
    ):
        arrive(ref, send_sem.at[phase])


def local(nx, *args):
    (
        tokens, mix_gain, w_gate, w_value, w_key, w_query, w_step, step_bias, decay_log, skip_gain,
        conv_x, conv_b, conv_c, window_x, window_b, window_c, state, head_gain, w_out, ffn_gain,
        route_ids, route_weights, e_gate, e_up, e_down,
    ) = args
    ne, nt = lax.axis_size("ep"), lax.axis_size("tp")
    rows = tokens.shape[0]
    half = rows // 2
    width = nt * HEAD_DIM
    experts = EXP_IN * ne
    operands = (
        tokens, mix_gain[None], w_gate.T, w_value.T, w_key, w_query, w_step.T,
        step_bias[None], decay_log[None], skip_gain[None],
        conv_x, conv_b, conv_c,
        window_x.transpose(1, 0, 2), window_b.transpose(1, 0, 2), window_c.transpose(1, 0, 2),
        state.reshape(rows * HEAD_DIM, STATE), head_gain[None], w_out, ffn_gain[None],
        route_ids.T, route_weights.T, e_gate[0], e_up[0], e_down[0],
    )
    eh = ne // 2
    hidden = e_gate.shape[2]
    vmem = pltpu.VMEM
    scratch = [
        vmem((rows, HEAD_DIM), BF16), vmem((1, width), F32), vmem((2 * HEAD_DIM + nt, width), BF16),
        vmem((width, 2 * STATE + 2 * HEAD_DIM + nt), BF16), vmem((1, nt), F32), vmem((1, nt), F32), vmem((1, nt), F32),
        vmem((4, HEAD_DIM), BF16), vmem((4, STATE), BF16), vmem((4, STATE), BF16),
        vmem((3, rows, HEAD_DIM), BF16), vmem((3, rows, STATE), BF16), vmem((3, rows, STATE), BF16),
        vmem((rows * HEAD_DIM, STATE), F32), vmem((1, HEAD_DIM), F32), vmem((HEAD_DIM, width), BF16),
        vmem((1, width), F32), vmem((2, rows), jnp.int32), vmem((2, rows), F32),
        vmem((width, 2 * hidden), BF16), vmem((hidden, width), BF16),
        vmem((half, 128), BF16), vmem((nt, half, 128), BF16),
        vmem((nt, half, 128), BF16), vmem((nt, half, 128), BF16),
        vmem((ne, EXP_IN, 128), F32), vmem((ne, EXP_IN, 128), BF16), vmem((ne, EXP_IN, 128), BF16),
        vmem((eh, EXP_IN, 128), F32),
        vmem((2, EXP_IN, eh, 128), BF16), vmem((2, nt, eh, 128), BF16),
        vmem((2, nt, eh, 128), BF16), vmem((2, nt, eh, 128), BF16),
        vmem((eh, EXP_IN, 128), F32), vmem((ne, EXP_IN, 128), BF16), vmem((ne, EXP_IN, 128), BF16),
        vmem((max(rows, 2 * eh), width), F32), vmem((max(rows, 2 * eh), width), BF16),
        vmem((STATE, rows * HEAD_DIM), BF16), vmem((STATE, rows * HEAD_DIM), BF16),
        vmem((experts, 2 * rows), BF16), vmem((2 * rows, 2 * experts), BF16),
        pltpu.SemaphoreType.DMA((25,)), pltpu.SemaphoreType.DMA((8,)),
        pltpu.SemaphoreType.DMA((4, nt // nx)), pltpu.SemaphoreType.DMA((5,)),
        pltpu.SemaphoreType.REGULAR, pltpu.SemaphoreType.REGULAR, pltpu.SemaphoreType.REGULAR,
    ]
    total = pl.pallas_call(
        functools.partial(kernel, ne, nt, nx, rows),
        out_shape=pltpu.VMEM((rows, HEAD_DIM), F32),
        in_specs=[pl.BlockSpec(memory_space=pl.ANY)] * len(operands),
        out_specs=pl.BlockSpec(memory_space=pltpu.VMEM),
        scratch_shapes=scratch,
        compiler_params=pltpu.CompilerParams(
            collective_id=0, has_side_effects=True
        ),
    )(*operands)
    return total.astype(BF16)


def solution(mesh):
    in_specs = (
        P("ep", "tp"), P(), P(None, "tp"), P(None, "tp"), P(), P(), P(), P(), P(), P(),
        P(None, "tp"), P(), P(), P("ep", None, "tp"), P("ep", None, None), P("ep", None, None),
        P("ep", "tp", None, None), P("tp"), P("tp", None), P(), P("ep", None), P("ep", None),
        P("ep", None, "tp"), P("ep", None, "tp"), P("ep", "tp", None),
    )
    return jax.shard_map(
        functools.partial(local, NX), mesh=mesh, in_specs=in_specs, out_specs=P("ep", "tp"), check_vma=False
    )
```
